32 devices in a mesh: grp: 2 (over x), sp: 4 (over y, core), tp: 4 (over z).
Axes of the slice: x: 2, y: 2, z: 4, core: 2. Of those that a mesh axis runs over, the one named last changes fastest.
Arguments:
- tokens: bfloat16 [8, 1024, 2048], P(('grp', 'tp'), 'sp'), parts along dimension 0, may hold values from -6 to 6
- kv_down: bfloat16 [2048, 512], replicated, may hold values from -0.125 to 0.125
- rope_down: bfloat16 [2048, 64], replicated, may hold values from -0.125 to 0.125
- kv_gain: float32 [512], replicated, may hold values from 0.1 to 1.9
- key_up: bfloat16 [512, 16, 128], replicated, may hold values from -0.25 to 0.25
- value_up: bfloat16 [512, 16, 128], replicated, may hold values from -0.25 to 0.25
- query_nope: bfloat16 [8, 16, 128], P(('grp', 'sp'), 'tp'), parts along dimension 0, may hold values from -180 to 180
- query_rope: bfloat16 [8, 16, 64], P(('grp', 'sp'), 'tp'), parts along dimension 0, may hold values from -180 to 180
Outputs:
- key_cache: bfloat16 [8, 16, 1024, 128], P(('grp', 'sp'), 'tp'), parts along dimension 0
- value_cache: bfloat16 [8, 16, 1024, 128], P(('grp', 'sp'), 'tp'), parts along dimension 0
- rope_cache: bfloat16 [8, 1024, 64], P(('grp', 'sp')), parts along dimension 0
- read_out: bfloat16 [8, 16, 128], P(('grp', 'sp'), 'tp'), parts along dimension 0
The draws below stay inside these ranges and needn't reach their ends.
There are 2 independent parts, one for each index of `grp`. The reference program is written for one: setup_inputs(seed, part) draws one part's arguments, and reference() takes and returns one part's arrays. A program takes and returns all parts, laid end to end along the dimension named above; an argument that names none is the same for every part. Nothing has to cross between parts.
All inputs are finite; a program needn't handle non-finite values.
Results may differ from the reference program's by a relative error of at most 0.018.
The reference program's roundings to bfloat16 on the way (of `normed` and `rotated`) count: a program that leaves them out, or rounds other values in their place, can miss the bound.
Values may be sent and summed in bfloat16 or wider, within the bound.
No kernel may reach another device: no remote copies, remote signals or barrier semaphores. Data moves between devices by JAX's collectives and lax.ppermute only.
A program may use at most 64 MiB of HBM per device.

```python
import jax
import jax.numpy as jnp
from jax import lax

D = 2048
HEADS = 16
KVL = 512
NOPE = 128
ROPE = 64
VD = 128
SEQS = 4
LEN = 1024


def query_draw(key, width):
    base = jax.random.normal(jax.random.fold_in(key, 11), (SEQS, HEADS, width), jnp.float32)
    base = jnp.clip(base, -6.0, 6.0)
    return base.astype(jnp.bfloat16)


def draw_query_nope(key, part):
    return query_draw(jax.random.fold_in(key, 1), NOPE)


def draw_query_rope(key, part):
    return query_draw(jax.random.fold_in(key, 2), ROPE)


def steps_of(key, shape, shards, least, high):
    loudness = 1.0
    for dim, blocks in shards:
        heights = jax.random.uniform(jax.random.fold_in(jax.random.fold_in(key, 6), dim), (blocks,), jnp.float32, least / len(shards), high / len(shards))
        loudness = loudness * jnp.repeat(jnp.exp(heights), shape[dim] // blocks).reshape((-1,) + (1,) * (len(shape) - 1 - dim))
    return loudness


def noise(stream_key, shape, scale, limit, pieces=(), kind=jnp.bfloat16):
    values = scale * jax.random.normal(stream_key, shape, jnp.float32)
    if pieces:
        values = values * steps_of(stream_key, shape, pieces, -0.22, 0.18)
    return jnp.clip(values, -limit, limit).astype(kind)


def setup_inputs(seed: int = 0, part: int = 0) -> dict:
    arg_keys = jax.random.split(jax.random.key(seed), 9)
    part_keys = jax.random.split(jax.random.fold_in(arg_keys[8], part), 9)
    return {
        "tokens": noise(part_keys[0], (SEQS, LEN, D), 1.0, 6.0, ((0, 4), (1, 4))),
        "kv_down": noise(arg_keys[1], (D, KVL), D ** -0.5, 0.125),
        "rope_down": noise(arg_keys[2], (D, ROPE), D ** -0.5, 0.125),
        "kv_gain": jnp.clip(1.0 + 0.18 * jax.random.normal(arg_keys[3], (KVL,), jnp.float32), 0.1, 1.9),
        "key_up": noise(arg_keys[4], (KVL, HEADS, NOPE), KVL ** -0.5, 0.25),
        "value_up": noise(arg_keys[5], (KVL, HEADS, VD), KVL ** -0.5, 0.25),
        "query_nope": draw_query_nope(jax.random.fold_in(jax.random.fold_in(arg_keys[8], part), 71), part),
        "query_rope": draw_query_rope(jax.random.fold_in(jax.random.fold_in(arg_keys[8], part), 71), part),
    }


norm_epsilon = 1e-06
rope_base = 10000.0

def rotate(values, positions):
    half_width = values.shape[-1] // 2
    frequency = 1.0 / rope_base ** (jnp.arange(0, 2 * half_width, 2, dtype=jnp.float32) / (2 * half_width))
    angles = positions[..., None] * frequency
    cosine = jnp.cos(angles)
    sine_part = jnp.sin(angles)
    front_half = values[..., :half_width]
    back_half = values[..., half_width:]
    return jnp.concatenate([front_half * cosine - back_half * sine_part, front_half * sine_part + back_half * cosine], axis=-1)

def reference(tokens, kv_down, rope_down, kv_gain, key_up, value_up, query_nope, query_rope):
    positions = jnp.arange(LEN, dtype=jnp.float32)
    key_flat = key_up.reshape(KVL, HEADS * NOPE)
    value_flat = value_up.reshape(KVL, HEADS * VD)

    def one_sequence(seq_rows):
        latent = jnp.dot(seq_rows, kv_down, preferred_element_type=jnp.float32)
        normed = (latent * lax.rsqrt(lax.optimization_barrier(jnp.mean(latent * latent, axis=-1, keepdims=True)) + norm_epsilon) * kv_gain).astype(jnp.bfloat16)
        rope_raw = jnp.dot(seq_rows, rope_down, preferred_element_type=jnp.float32)
        rope_key = rotate(rope_raw, positions).astype(jnp.bfloat16)
        key_rows = jnp.dot(normed, key_flat, preferred_element_type=jnp.float32).astype(jnp.bfloat16)
        value_rows = jnp.dot(normed, value_flat, preferred_element_type=jnp.float32).astype(jnp.bfloat16)
        key_rows = key_rows.reshape(LEN, HEADS, NOPE).transpose(1, 0, 2)
        value_rows = value_rows.reshape(LEN, HEADS, VD).transpose(1, 0, 2)
        return (key_rows, value_rows, rope_key)
    key_cache, value_cache, rope_cache = lax.map(one_sequence, tokens)
    query_pos = jnp.full((HEADS,), LEN, dtype=jnp.float32)
    rotated = rotate(query_rope.astype(jnp.float32), query_pos).astype(jnp.bfloat16)
    score_scale = (NOPE + ROPE) ** (-0.5)
    scores = jnp.einsum('shd,shld->shl', query_nope.astype(jnp.float32), key_cache.astype(jnp.float32))
    scores = scores + jnp.einsum('shr,slr->shl', rotated.astype(jnp.float32), rope_cache.astype(jnp.float32))
    scores = scores * score_scale
    row_max = lax.optimization_barrier(jnp.max(scores, axis=-1, keepdims=True))
    expo_terms = jnp.exp(scores - row_max)
    weights = expo_terms / lax.optimization_barrier(jnp.sum(expo_terms, axis=-1, keepdims=True))
    read_out = jnp.einsum('shl,shld->shd', weights, value_cache.astype(jnp.float32)).astype(jnp.bfloat16)
    return (key_cache, value_cache, rope_cache, read_out)
```

```python
import functools

import jax
import jax.numpy as jnp
import numpy as np
from jax import lax
from jax.experimental import pallas as pl
from jax.experimental.pallas import tpu as pltpu
from jax.sharding import PartitionSpec as P

norm_epsilon = 1e-06
rope_base = 10000.0
f32, bf16 = jnp.float32, jnp.bfloat16
ANY = pl.BlockSpec(memory_space=pl.ANY)
VMEM = pl.BlockSpec(memory_space=pltpu.VMEM)
SMEM = pl.BlockSpec(memory_space=pltpu.SMEM)


def frequencies(half):
    exponent = np.arange(0, 2 * half, 2, dtype=np.float32) / np.float32(2 * half)
    return (np.float32(1.0) / np.power(np.float32(rope_base), exponent)).astype(np.float32)


def project_kernel(chunks, at, x, w, r, gain, freq, out, xs, ws, rs, sems):
    seqs, pos, width = x.shape
    half = r.shape[0] // 2
    step = width // chunks
    copies = []
    for c in range(chunks):
        part = pl.ds(c * step, step)
        copies.append(pltpu.make_async_copy(w.at[part], ws.at[part], sems.at[0, c]))
        copies.append(pltpu.make_async_copy(x.at[:, :, part], xs.at[:, :, part], sems.at[1, c]))
        copies[-2].start()
        copies[-1].start()
    rope_copy = pltpu.make_async_copy(r, rs, sems.at[2, 0])
    rope_copy.start()
    places = at[0] * pos + lax.broadcasted_iota(jnp.int32, (half, pos), 1)
    angles = places.astype(f32) * freq[:, :1]
    cosine, sine = jnp.cos(angles), jnp.sin(angles)
    latents = [None] * seqs
    for c in range(chunks):
        copies[2 * c].wait()
        copies[2 * c + 1].wait()
        for s in range(seqs):
            term = jnp.dot(
                xs[s, :, c * step : (c + 1) * step],
                ws[c * step : (c + 1) * step, :],
                preferred_element_type=f32,
            )
            latents[s] = term if c == 0 else latents[s] + term
    rope_copy.wait()
    for s in range(seqs):
        latent = latents[s]
        square = jnp.mean(latent * latent, axis=-1, keepdims=True)
        normed = latent * lax.rsqrt(square + norm_epsilon) * gain[...]
        out[s, :pos, :] = normed.astype(bf16)
        raw = lax.dot_general(
            rs[...], xs[s], (((1,), (1,)), ((), ())), preferred_element_type=f32
        )
        front, back = raw[:half], raw[half:]
        out[s, pos:, :pos] = (front * cosine - back * sine).astype(bf16)
        out[s, pos:, pos : 2 * pos] = (front * sine + back * cosine).astype(bf16)


def project(tokens, kv_down, rope_t, gain, sp_index):
    seqs, pos, width = tokens.shape
    latent = kv_down.shape[1]
    half = rope_t.shape[0] // 2
    assert 2 * pos == latent
    chunks = 4
    freq = jnp.asarray(np.broadcast_to(frequencies(half)[:, None], (half, 128)))
    return pl.pallas_call(
        functools.partial(project_kernel, chunks),
        out_shape=jax.ShapeDtypeStruct((seqs, pos + half, latent), bf16),
        in_specs=[SMEM, ANY, ANY, ANY, VMEM, VMEM],
        out_specs=VMEM,
        scratch_shapes=[
            pltpu.VMEM(tokens.shape, bf16),
            pltpu.VMEM(kv_down.shape, bf16),
            pltpu.VMEM(rope_t.shape, bf16),
            pltpu.SemaphoreType.DMA((3, chunks)),
        ],
        name="project",
        cost_estimate=pl.CostEstimate(
            flops=2 * seqs * pos * width * (latent + 2 * half),
            bytes_accessed=2 * (tokens.size + kv_down.size + seqs * pos * latent),
            transcendentals=0,
        ),
    )(sp_index[None], tokens, kv_down, rope_t, gain[None], freq)


def absorb_kernel(first, last, heads, scale, at, *refs):
    block, w, q, qr, refs = refs[0], refs[1], refs[2], refs[3], refs[4:]
    if not first:
        state, refs = refs[0], refs[4:]
    keys, values, ropes, end, kv, rope, sems = refs
    half = qr.shape[1] // 2
    pos = block.shape[0] - half
    wide = w.shape[1] // 2
    head = wide // heads
    place = pl.ds(at[0] * pos, pos)
    rope[:half] = block[pos:, :pos]
    rope[half:] = block[pos:, pos : 2 * pos]
    copies = [pltpu.make_async_copy(rope, ropes.at[:, place], sems.at[2 * heads])]
    copies[0].start()
    x = block[:pos]
    made = []
    for i, cache in enumerate((keys, values)):
        both = jnp.dot(x, w[:, i * wide : (i + 1) * wide], preferred_element_type=f32)
        both = both.astype(bf16)
        made.append(both)
        for h in range(heads):
            n = i * heads + h
            kv[n] = both[:, h * head : (h + 1) * head]
            copies.append(pltpu.make_async_copy(kv.at[n], cache.at[h, place], sems.at[n]))
            copies[-1].start()
    k, v = made
    scores = lax.dot_general(q[...], k, (((1,), (1,)), ((), ())), preferred_element_type=f32)
    scores = scores + jnp.dot(qr[...], rope[...], preferred_element_type=f32)
    scores = scores * scale
    peak = jnp.max(scores, axis=-1, keepdims=True)
    if not first:
        old_peak = state[0, :, :1]
        peak = jnp.maximum(peak, old_peak)
    terms = jnp.exp(scores - peak)
    total = jnp.sum(terms, axis=-1, keepdims=True)
    high = terms.astype(bf16)
    low = (terms - high.astype(f32)).astype(bf16)
    read = jnp.dot(high, v, preferred_element_type=f32) + jnp.dot(
        low, v, preferred_element_type=f32
    )
    row = lax.broadcasted_iota(jnp.int32, (heads, 1), 0)
    mine = jnp.zeros((heads, head), f32)
    for h in range(heads):
        mine = mine + jnp.where(row == h, read[:, h * head : (h + 1) * head], 0.0)
    if not first:
        fade = jnp.exp(old_peak - peak)
        total = total + fade * state[1, :, :1]
        mine = mine + fade * state[2]
    if last:
        end[...] = (mine / total).astype(bf16)
    else:
        end[0] = jnp.broadcast_to(peak, mine.shape)
        end[1] = jnp.broadcast_to(total, mine.shape)
        end[2] = mine
    for copy in copies:
        copy.wait()


def absorb(first, last, blocks, heads, scale, at, block, w, q, qr, held):
    latent = w.shape[0]
    half = qr.shape[1] // 2
    pos = block.shape[0] - half
    head = w.shape[1] // (2 * heads)
    caches = [
        jax.ShapeDtypeStruct((heads, blocks * pos, head), bf16),
        jax.ShapeDtypeStruct((heads, blocks * pos, head), bf16),
        jax.ShapeDtypeStruct((2 * half, blocks * pos), bf16),
    ]
    end = jax.ShapeDtypeStruct((heads, head), bf16) if last else jax.ShapeDtypeStruct(
        (3, heads, head), f32
    )
    extra = [] if first else [held[3], *held[:3]]
    return pl.pallas_call(
        functools.partial(absorb_kernel, first, last, heads, scale),
        out_shape=[*caches, end],
        in_specs=[SMEM, VMEM, VMEM, VMEM, VMEM] + ([] if first else [VMEM, ANY, ANY, ANY]),
        out_specs=[ANY, ANY, ANY, VMEM],
        input_output_aliases={} if first else {6: 0, 7: 1, 8: 2},
        scratch_shapes=[
            pltpu.VMEM((2 * heads, pos, head), bf16),
            pltpu.VMEM((2 * half, pos), bf16),
            pltpu.SemaphoreType.DMA((2 * heads + 1,)),
        ],
        name="absorb",
        cost_estimate=pl.CostEstimate(
            flops=4 * pos * latent * heads * head,
            bytes_accessed=2 * (block.size + w.size) + 4 * pos * heads * head,
            transcendentals=heads * pos,
        ),
    )(at[None], block, w, q, qr, *extra)


def rotated_query(query_rope, position):
    half = query_rope.shape[-1] // 2
    angles = np.float32(position) * frequencies(half)
    cosine, sine = jnp.cos(jnp.asarray(angles)), jnp.sin(jnp.asarray(angles))
    front, back = query_rope[..., :half].astype(f32), query_rope[..., half:].astype(f32)
    turned = [front * cosine - back * sine, front * sine + back * cosine]
    return jnp.concatenate(turned, axis=-1).astype(bf16)


def local(sp_count, tp_count, tokens, kv_down, rope_down, kv_gain, key_up, value_up, query_nope, query_rope):
    seqs, pos, _ = tokens.shape
    assert seqs * tp_count == sp_count
    latent, head_count, key_width = key_up.shape
    heads = head_count // tp_count
    sp_index = lax.axis_index("sp")
    tp_index = lax.axis_index("tp")
    blocks = project(tokens, kv_down, rope_down.T, kv_gain, sp_index)

    mine = lax.rem(sp_index, seqs) * tp_count + tp_index
    arrived = []
    for k in range(sp_count):
        pairs = []
        for s in range(sp_count):
            for t in range(tp_count):
                source = ((s % seqs) * tp_count + t) ^ k
                pairs.append((source * tp_count + s // seqs, s * tp_count + t))
        if seqs == 1:
            block = blocks[0]
        else:
            block = lax.dynamic_index_in_dim(
                blocks, jnp.bitwise_xor(sp_index, k) // tp_count, 0, keepdims=False
            )
        arrived.append((jnp.bitwise_xor(mine, k), lax.ppermute(block, ("sp", "tp"), pairs)))

    start = tp_index * heads
    w = jnp.concatenate(
        [
            lax.dynamic_slice_in_dim(up, start, heads, 1).reshape(latent, -1)
            for up in (key_up, value_up)
        ],
        axis=1,
    )
    eye = jnp.eye(heads, dtype=bf16)
    q = (query_nope[0][:, None, :] * eye[:, :, None]).reshape(heads, heads * key_width)
    qr = rotated_query(query_rope[0], pos * sp_count)
    scale = (key_width + query_rope.shape[-1]) ** (-0.5)
    held = None
    for k, (at, block) in enumerate(arrived):
        held = absorb(
            k == 0, k == sp_count - 1, sp_count, heads, scale, at, block, w, q, qr, held
        )
    keys, values, ropes, read = held
    return keys[None], values[None], ropes.T[None], read[None]


def solution(mesh):
    placed = (
        P(("grp", "tp"), "sp", None),
        P(),
        P(),
        P(),
        P(),
        P(),
        P(("grp", "sp"), "tp", None),
        P(("grp", "sp"), "tp", None),
    )
    return jax.shard_map(
        functools.partial(local, mesh.shape["sp"], mesh.shape["tp"]),
        mesh=mesh,
        in_specs=placed,
        out_specs=(
            P(("grp", "sp"), "tp", None, None),
            P(("grp", "sp"), "tp", None, None),
            P(("grp", "sp"), None, None),
            P(("grp", "sp"), "tp", None),
        ),
        check_vma=False,
    )
```

```python
import functools

import jax
import jax.numpy as jnp
import numpy as np
from jax import lax
from jax.experimental import pallas as pl
from jax.experimental.pallas import tpu as pltpu
from jax.sharding import PartitionSpec as P

norm_epsilon = 1e-06
rope_base = 10000.0
f32, bf16 = jnp.float32, jnp.bfloat16
ANY = pl.BlockSpec(memory_space=pl.ANY)
VMEM = pl.BlockSpec(memory_space=pltpu.VMEM)
SMEM = pl.BlockSpec(memory_space=pltpu.SMEM)


def turns(positions, half):
    exponent = np.arange(0, 2 * half, 2, dtype=np.float32) / np.float32(2 * half)
    frequency = np.float32(1.0) / np.power(np.float32(rope_base), exponent)
    angles = frequency[:, None] * np.asarray(positions, np.float32)[None, :]
    return np.concatenate([np.cos(angles), np.sin(angles)]).astype(np.float32)


def project_kernel(chunks, at, x, w, r, gain, turn, out, xs, ws, rs, gs, ts, sems):
    seqs, pos, width = x.shape
    half = r.shape[0] // 2
    step = width // chunks
    copies = []
    for c in range(chunks):
        part = pl.ds(c * step, step)
        copies.append(pltpu.make_async_copy(w.at[part], ws.at[part], sems.at[c]))
        copies.append(pltpu.make_async_copy(x.at[:, :, part], xs.at[:, :, part], sems.at[chunks + c]))
    place = pl.ds(pl.multiple_of(at[0] * pos, pos), pos)
    copies.append(pltpu.make_async_copy(r, rs, sems.at[2 * chunks]))
    copies.append(pltpu.make_async_copy(gain, gs, sems.at[2 * chunks + 1]))
    copies.append(pltpu.make_async_copy(turn.at[:, place], ts, sems.at[2 * chunks + 2]))
    for copy in copies:
        copy.start()
    latents = [None] * seqs
    for c in range(chunks):
        copies[2 * c].wait()
        copies[2 * c + 1].wait()
        for s in range(seqs):
            term = jnp.dot(
                xs[s, :, c * step : (c + 1) * step],
                ws[c * step : (c + 1) * step, :],
                preferred_element_type=f32,
            )
            latents[s] = term if c == 0 else latents[s] + term
    for copy in copies[2 * chunks :]:
        copy.wait()
    cosine, sine = ts[:half], ts[half:]
    for s in range(seqs):
        latent = latents[s]
        square = jnp.mean(latent * latent, axis=-1, keepdims=True)
        normed = latent * lax.rsqrt(square + norm_epsilon) * gs[...]
        out[s, :pos, :] = normed.astype(bf16)
        raw = lax.dot_general(
            rs[...], xs[s], (((1,), (1,)), ((), ())), preferred_element_type=f32
        )
        front, back = raw[:half], raw[half:]
        out[s, pos:, :pos] = (front * cosine - back * sine).astype(bf16)
        out[s, pos:, pos : 2 * pos] = (front * sine + back * cosine).astype(bf16)


def project(tokens, kv_down, rope_t, gain, sp_index, sp_count):
    seqs, pos, width = tokens.shape
    latent = kv_down.shape[1]
    half = rope_t.shape[0] // 2
    assert 2 * pos == latent
    chunks = 4
    turn = jnp.asarray(turns(np.arange(pos * sp_count), half))
    return pl.pallas_call(
        functools.partial(project_kernel, chunks),
        out_shape=jax.ShapeDtypeStruct((seqs, pos + half, latent), bf16),
        in_specs=[SMEM, ANY, ANY, ANY, ANY, ANY],
        out_specs=VMEM,
        scratch_shapes=[
            pltpu.VMEM(tokens.shape, bf16),
            pltpu.VMEM(kv_down.shape, bf16),
            pltpu.VMEM(rope_t.shape, bf16),
            pltpu.VMEM((1, latent), f32),
            pltpu.VMEM((2 * half, pos), f32),
            pltpu.SemaphoreType.DMA((2 * chunks + 3,)),
        ],
        name="project",
        cost_estimate=pl.CostEstimate(
            flops=2 * seqs * pos * width * (latent + 2 * half),
            bytes_accessed=2 * (tokens.size + kv_down.size + seqs * pos * latent),
            transcendentals=0,
        ),
    )(sp_index[None], tokens, kv_down, rope_t, gain[None], turn)


def absorb_kernel(first, last, heads, scale, at, *refs):
    block, w, q, qr, refs = refs[0], refs[1], refs[2], refs[3], refs[4:]
    if not first:
        state, refs = refs[0], refs[4:]
    keys, values, ropes, end, kv, rope, sems = refs
    half = qr.shape[1] // 2
    pos = block.shape[0] - half
    wide = w.shape[1] // 2
    head = wide // heads
    place = pl.ds(at[0] * pos, pos)
    rope[:half] = block[pos:, :pos]
    rope[half:] = block[pos:, pos : 2 * pos]
    copies = [pltpu.make_async_copy(rope, ropes.at[:, place], sems.at[2 * heads])]
    copies[0].start()
    x = block[:pos]
    made = []
    for i, cache in enumerate((keys, values)):
        both = jnp.dot(x, w[:, i * wide : (i + 1) * wide], preferred_element_type=f32)
        both = both.astype(bf16)
        made.append(both)
        for h in range(heads):
            n = i * heads + h
            kv[n] = both[:, h * head : (h + 1) * head]
            copies.append(pltpu.make_async_copy(kv.at[n], cache.at[h, place], sems.at[n]))
            copies[-1].start()
    k, v = made
    scores = lax.dot_general(q[...], k, (((1,), (1,)), ((), ())), preferred_element_type=f32)
    scores = scores + jnp.dot(qr[...], rope[...], preferred_element_type=f32)
    scores = scores * scale
    peak = jnp.max(scores, axis=-1, keepdims=True)
    if not first:
        old_peak = state[0, :, :1]
        peak = jnp.maximum(peak, old_peak)
    terms = jnp.exp(scores - peak)
    total = jnp.sum(terms, axis=-1, keepdims=True)
    high = terms.astype(bf16)
    low = (terms - high.astype(f32)).astype(bf16)
    read = jnp.dot(high, v, preferred_element_type=f32) + jnp.dot(
        low, v, preferred_element_type=f32
    )
    row = lax.broadcasted_iota(jnp.int32, (heads, 1), 0)
    mine = jnp.zeros((heads, head), f32)
    for h in range(heads):
        mine = mine + jnp.where(row == h, read[:, h * head : (h + 1) * head], 0.0)
    if not first:
        fade = jnp.exp(old_peak - peak)
        total = total + fade * state[1, :, :1]
        mine = mine + fade * state[2]
    if last:
        end[...] = (mine / total).astype(bf16)
    else:
        end[0] = jnp.broadcast_to(peak, mine.shape)
        end[1] = jnp.broadcast_to(total, mine.shape)
        end[2] = mine
    for copy in copies:
        copy.wait()


def absorb(first, last, blocks, heads, scale, at, block, w, q, qr, held):
    latent = w.shape[0]
    half = qr.shape[1] // 2
    pos = block.shape[0] - half
    head = w.shape[1] // (2 * heads)
    caches = [
        jax.ShapeDtypeStruct((heads, blocks * pos, head), bf16),
        jax.ShapeDtypeStruct((heads, blocks * pos, head), bf16),
        jax.ShapeDtypeStruct((2 * half, blocks * pos), bf16),
    ]
    end = jax.ShapeDtypeStruct((heads, head), bf16) if last else jax.ShapeDtypeStruct(
        (3, heads, head), f32
    )
    extra = [] if first else [held[3], *held[:3]]
    return pl.pallas_call(
        functools.partial(absorb_kernel, first, last, heads, scale),
        out_shape=[*caches, end],
        in_specs=[SMEM, VMEM, VMEM, VMEM, VMEM] + ([] if first else [VMEM, ANY, ANY, ANY]),
        out_specs=[ANY, ANY, ANY, VMEM],
        input_output_aliases={} if first else {6: 0, 7: 1, 8: 2},
        scratch_shapes=[
            pltpu.VMEM((2 * heads, pos, head), bf16),
            pltpu.VMEM((2 * half, pos), bf16),
            pltpu.SemaphoreType.DMA((2 * heads + 1,)),
        ],
        compiler_params=pltpu.CompilerParams(vmem_limit_bytes=8 * 2**20),
        name="absorb",
        cost_estimate=pl.CostEstimate(
            flops=4 * pos * latent * heads * head,
            bytes_accessed=2 * (block.size + w.size) + 4 * pos * heads * head,
            transcendentals=heads * pos,
        ),
    )(at[None], block, w, q, qr, *extra)


def rotated_query(query_rope, position):
    half = query_rope.shape[-1] // 2
    turn = turns([position], half)[:, 0]
    cosine, sine = jnp.asarray(turn[:half]), jnp.asarray(turn[half:])
    front, back = query_rope[..., :half].astype(f32), query_rope[..., half:].astype(f32)
    turned = [front * cosine - back * sine, front * sine + back * cosine]
    return jnp.concatenate(turned, axis=-1).astype(bf16)


def local(sp_count, tp_count, tokens, kv_down, rope_down, kv_gain, key_up, value_up, query_nope, query_rope):
    seqs, pos, _ = tokens.shape
    assert seqs * tp_count == sp_count
    latent, head_count, key_width = key_up.shape
    heads = head_count // tp_count
    sp_index = lax.axis_index("sp")
    tp_index = lax.axis_index("tp")
    blocks = project(tokens, kv_down, rope_down.T, kv_gain, sp_index, sp_count)

    mine = lax.rem(sp_index, seqs) * tp_count + tp_index
    arrived = []
    for k in range(sp_count):
        pairs = []
        for s in range(sp_count):
            for t in range(tp_count):
                source = ((s % seqs) * tp_count + t - k) % sp_count
                pairs.append((source * tp_count + s // seqs, s * tp_count + t))
        if seqs == 1:
            block = blocks[0]
        else:
            block = lax.dynamic_index_in_dim(
                blocks, lax.rem(sp_index + k, sp_count) // tp_count, 0, keepdims=False
            )
        arrived.append((lax.rem(mine + sp_count - k, sp_count), lax.ppermute(block, ("sp", "tp"), pairs)))

    start = tp_index * heads
    w = jnp.concatenate(
        [
            lax.dynamic_slice_in_dim(up, start, heads, 1).reshape(latent, -1)
            for up in (key_up, value_up)
        ],
        axis=1,
    )
    eye = jnp.eye(heads, dtype=bf16)
    q = (query_nope[0][:, None, :] * eye[:, :, None]).reshape(heads, heads * key_width)
    qr = rotated_query(query_rope[0], pos * sp_count)
    scale = (key_width + query_rope.shape[-1]) ** (-0.5)
    held = None
    for k, (at, block) in enumerate(arrived):
        held = absorb(
            k == 0, k == sp_count - 1, sp_count, heads, scale, at, block, w, q, qr, held
        )
    keys, values, ropes, read = held
    return keys[None], values[None], ropes.T[None], read[None]


def solution(mesh):
    placed = (
        P(("grp", "tp"), "sp", None),
        P(),
        P(),
        P(),
        P(),
        P(),
        P(("grp", "sp"), "tp", None),
        P(("grp", "sp"), "tp", None),
    )
    return jax.shard_map(
        functools.partial(local, mesh.shape["sp"], mesh.shape["tp"]),
        mesh=mesh,
        in_specs=placed,
        out_specs=(
            P(("grp", "sp"), "tp", None, None),
            P(("grp", "sp"), "tp", None, None),
            P(("grp", "sp"), None, None),
            P(("grp", "sp"), "tp", None),
        ),
        check_vma=False,
    )
```

```python
import functools

import jax
import jax.numpy as jnp
import numpy as np
from jax import lax
from jax.experimental import pallas as pl
from jax.experimental.pallas import tpu as pltpu
from jax.sharding import PartitionSpec as P

norm_epsilon = 1e-06
rope_base = 10000.0
f32, bf16 = jnp.float32, jnp.bfloat16
ANY = pl.BlockSpec(memory_space=pl.ANY)
VMEM = pl.BlockSpec(memory_space=pltpu.VMEM)
SMEM = pl.BlockSpec(memory_space=pltpu.SMEM)


def turns(positions, half):
    exponent = np.arange(0, 2 * half, 2, dtype=np.float32) / np.float32(2 * half)
    frequency = np.float32(1.0) / np.power(np.float32(rope_base), exponent)
    angles = frequency[:, None] * np.asarray(positions, np.float32)[None, :]
    return np.concatenate([np.cos(angles), np.sin(angles)]).astype(np.float32)


def project_kernel(chunks, at, x, w, r, gain, turn, out, xs, ws, rs, gs, ts, sems):
    seqs, pos, width = x.shape
    half = r.shape[0] // 2
    step = width // chunks
    copies = []
    for c in range(chunks):
        part = pl.ds(c * step, step)
        copies.append(pltpu.make_async_copy(w.at[part], ws.at[part], sems.at[c]))
        copies.append(pltpu.make_async_copy(x.at[:, :, part], xs.at[:, :, part], sems.at[chunks + c]))
    place = pl.ds(pl.multiple_of(at[0] * pos, pos), pos)
    copies.append(pltpu.make_async_copy(r, rs, sems.at[2 * chunks]))
    copies.append(pltpu.make_async_copy(gain, gs, sems.at[2 * chunks + 1]))
    copies.append(pltpu.make_async_copy(turn.at[:, place], ts, sems.at[2 * chunks + 2]))
    for copy in copies:
        copy.start()
    latents = [None] * seqs
    for c in range(chunks):
        copies[2 * c].wait()
        copies[2 * c + 1].wait()
        for s in range(seqs):
            term = jnp.dot(
                xs[s, :, c * step : (c + 1) * step],
                ws[c * step : (c + 1) * step, :],
                preferred_element_type=f32,
            )
            latents[s] = term if c == 0 else latents[s] + term
    for copy in copies[2 * chunks :]:
        copy.wait()
    cosine, sine = ts[:half], ts[half:]
    for s in range(seqs):
        latent = latents[s]
        square = jnp.mean(latent * latent, axis=-1, keepdims=True)
        normed = latent * lax.rsqrt(square + norm_epsilon) * gs[...]
        out[s, :pos, :] = normed.astype(bf16)
        raw = lax.dot_general(
            rs[...], xs[s], (((1,), (1,)), ((), ())), preferred_element_type=f32
        )
        front, back = raw[:half], raw[half:]
        out[s, pos:, :pos] = (front * cosine - back * sine).astype(bf16)
        out[s, pos:, pos : 2 * pos] = (front * sine + back * cosine).astype(bf16)


def project(tokens, kv_down, rope_t, gain, sp_index, sp_count):
    seqs, pos, width = tokens.shape
    latent = kv_down.shape[1]
    half = rope_t.shape[0] // 2
    assert 2 * pos == latent
    chunks = 4
    turn = jnp.asarray(turns(np.arange(pos * sp_count), half))
    return pl.pallas_call(
        functools.partial(project_kernel, chunks),
        out_shape=jax.ShapeDtypeStruct((seqs, pos + half, latent), bf16),
        in_specs=[SMEM, ANY, ANY, ANY, ANY, ANY],
        out_specs=VMEM,
        scratch_shapes=[
            pltpu.VMEM(tokens.shape, bf16),
            pltpu.VMEM(kv_down.shape, bf16),
            pltpu.VMEM(rope_t.shape, bf16),
            pltpu.VMEM((1, latent), f32),
            pltpu.VMEM((2 * half, pos), f32),
            pltpu.SemaphoreType.DMA((2 * chunks + 3,)),
        ],
        name="project",
        cost_estimate=pl.CostEstimate(
            flops=2 * seqs * pos * width * (latent + 2 * half),
            bytes_accessed=2 * (tokens.size + kv_down.size + seqs * pos * latent),
            transcendentals=0,
        ),
    )(sp_index[None], tokens, kv_down, rope_t, gain[None], turn)


def absorb_kernel(first, last, two, heads, scale, at, *refs):
    block, refs = refs[0], refs[1:]
    if two:
        other, refs = refs[0], refs[1:]
    w, q, qr, refs = refs[0], refs[1], refs[2], refs[3:]
    if not first:
        state, refs = refs[0], refs[4:]
    keys, values, ropes, end, kv, rope, read_out, sems = refs
    half = qr.shape[1] // 2
    pos = block.shape[0] - half
    wide = w.shape[1] // 2
    head = wide // heads
    place = pl.ds(pl.multiple_of(at[0] * pos, pos), pos)
    held = block[...]
    if two:
        held = jnp.where(at[1] == 1, other[...], held)
    rope[:half] = held[pos:, :pos]
    rope[half:] = held[pos:, pos : 2 * pos]
    copies = [pltpu.make_async_copy(rope, ropes.at[:, place], sems.at[2 * heads])]
    copies[0].start()
    x = held[:pos]
    made = []
    for i, cache in enumerate((keys, values)):
        both = jnp.dot(x, w[:, i * wide : (i + 1) * wide], preferred_element_type=f32)
        both = both.astype(bf16)
        made.append(both)
        for h in range(heads):
            n = i * heads + h
            kv[n] = both[:, h * head : (h + 1) * head]
            copies.append(pltpu.make_async_copy(kv.at[n], cache.at[h, place], sems.at[n]))
            copies[-1].start()
    k, v = made
    scores = lax.dot_general(q[...], k, (((1,), (1,)), ((), ())), preferred_element_type=f32)
    scores = scores + jnp.dot(qr[...], rope[...], preferred_element_type=f32)
    scores = scores * scale
    peak = jnp.max(scores, axis=-1, keepdims=True)
    if not first:
        old_peak = state[0, :, :1]
        peak = jnp.maximum(peak, old_peak)
    terms = jnp.exp(scores - peak)
    total = jnp.sum(terms, axis=-1, keepdims=True)
    high = terms.astype(bf16)
    low = (terms - high.astype(f32)).astype(bf16)
    read = jnp.dot(high, v, preferred_element_type=f32) + jnp.dot(
        low, v, preferred_element_type=f32
    )
    row = lax.broadcasted_iota(jnp.int32, (heads, 1), 0)
    mine = jnp.zeros((heads, head), f32)
    for h in range(heads):
        mine = mine + jnp.where(row == h, read[:, h * head : (h + 1) * head], 0.0)
    if not first:
        fade = jnp.exp(old_peak - peak)
        total = total + fade * state[1, :, :1]
        mine = mine + fade * state[2]
    if last:
        read_out[...] = (mine / total).astype(bf16)
        copies.append(pltpu.make_async_copy(read_out, end, sems.at[2 * heads + 1]))
        copies[-1].start()
    else:
        end[0] = jnp.broadcast_to(peak, mine.shape)
        end[1] = jnp.broadcast_to(total, mine.shape)
        end[2] = mine
    for copy in copies:
        copy.wait()


def absorb(first, last, blocks, heads, scale, at, either, w, q, qr, held):
    latent = w.shape[0]
    half = qr.shape[1] // 2
    pos = either[0].shape[0] - half
    head = w.shape[1] // (2 * heads)
    caches = [
        jax.ShapeDtypeStruct((heads, blocks * pos, head), bf16),
        jax.ShapeDtypeStruct((heads, blocks * pos, head), bf16),
        jax.ShapeDtypeStruct((2 * half, blocks * pos), bf16),
    ]
    end = jax.ShapeDtypeStruct((heads, head), bf16) if last else jax.ShapeDtypeStruct(
        (3, heads, head), f32
    )
    extra = [] if first else [held[3], *held[:3]]
    base = 4 + len(either) + 1
    return pl.pallas_call(
        functools.partial(absorb_kernel, first, last, len(either) == 2, heads, scale),
        out_shape=[*caches, end],
        in_specs=[SMEM]
        + [VMEM] * (len(either) + 3)
        + ([] if first else [VMEM, ANY, ANY, ANY]),
        out_specs=[ANY, ANY, ANY, ANY if last else VMEM],
        input_output_aliases={} if first else {base: 0, base + 1: 1, base + 2: 2},
        scratch_shapes=[
            pltpu.VMEM((2 * heads, pos, head), bf16),
            pltpu.VMEM((2 * half, pos), bf16),
            pltpu.VMEM((heads, head), bf16),
            pltpu.SemaphoreType.DMA((2 * heads + 2,)),
        ],
        compiler_params=pltpu.CompilerParams(vmem_limit_bytes=8 * 2**20),
        name="absorb",
        cost_estimate=pl.CostEstimate(
            flops=4 * pos * latent * heads * head,
            bytes_accessed=2 * (either[0].size + w.size) + 4 * pos * heads * head,
            transcendentals=heads * pos,
        ),
    )(at, *either, w, q, qr, *extra)


def rotated_query(query_rope, position):
    half = query_rope.shape[-1] // 2
    turn = turns([position], half)[:, 0]
    cosine, sine = jnp.asarray(turn[:half]), jnp.asarray(turn[half:])
    front, back = query_rope[..., :half].astype(f32), query_rope[..., half:].astype(f32)
    turned = [front * cosine - back * sine, front * sine + back * cosine]
    return jnp.concatenate(turned, axis=-1).astype(bf16)


def local(sp_count, tp_count, tokens, kv_down, rope_down, kv_gain, key_up, value_up, query_nope, query_rope):
    seqs, pos, _ = tokens.shape
    assert seqs * tp_count == sp_count and sp_count % 2 == 0
    latent, head_count, key_width = key_up.shape
    heads = head_count // tp_count
    sp_index = lax.axis_index("sp")
    tp_index = lax.axis_index("tp")
    blocks = project(tokens, kv_down, rope_down.T, kv_gain, sp_index, sp_count)

    fold = sp_count // 2
    relay = seqs == 1 and sp_count == 4
    my_spot = lax.rem(sp_index, seqs) * tp_count + tp_index
    my_rank = lax.rem(sp_index, 2) * fold + sp_index // 2
    arrived, places = [], []
    for k in range(sp_count):
        pairs = []
        for s in range(sp_count):
            for t in range(tp_count):
                turn = (2 - k) * (1 - s // seqs % 2 * 2)
                rank = ((s % seqs) * tp_count + t - turn) % sp_count
                source = rank % fold * 2 + rank // fold
                if not (relay and k == 3 and t == s ^ 3):
                    pairs.append((source * tp_count + s // seqs, s * tp_count + t))
        if seqs == 1:
            block = blocks[0]
        else:
            turn = (2 - k) * (1 - lax.rem(tp_index, 2) * 2)
            block = lax.dynamic_index_in_dim(
                blocks, jnp.mod(my_rank + turn, sp_count) // tp_count, 0, keepdims=False
            )
        arrived.append(lax.ppermute(block, ("sp", "tp"), pairs))
        turn = (2 - k) * (1 - lax.rem(sp_index // seqs, 2) * 2)
        rank = lax.rem(my_spot + 2 * sp_count - turn, sp_count)
        places.append(lax.rem(rank, fold) * 2 + rank // fold)
    if relay:
        pairs = [(s * tp_count + (s ^ 2), s * tp_count + (s ^ 3)) for s in range(4)]
        relayed = lax.ppermute(arrived[0], ("sp", "tp"), pairs)
        from_relay = (tp_index == jnp.bitwise_xor(sp_index, 3)).astype(jnp.int32)

    start = tp_index * heads
    w = jnp.concatenate(
        [
            lax.dynamic_slice_in_dim(up, start, heads, 1).reshape(latent, -1)
            for up in (key_up, value_up)
        ],
        axis=1,
    )
    eye = jnp.eye(heads, dtype=bf16)
    q = (query_nope[0][:, None, :] * eye[:, :, None]).reshape(heads, heads * key_width)
    qr = rotated_query(query_rope[0], pos * sp_count)
    scale = (key_width + query_rope.shape[-1]) ** (-0.5)
    held = None
    for k, (place, block) in enumerate(zip(places, arrived)):
        last = k == sp_count - 1
        either = [block]
        at = place[None]
        if last and relay:
            either.append(relayed)
            at = jnp.stack([place, from_relay])
        held = absorb(k == 0, last, sp_count, heads, scale, at, either, w, q, qr, held)
    keys, values, ropes, read = held
    return keys[None], values[None], ropes.T[None], read[None]


def solution(mesh):
    placed = (
        P(("grp", "tp"), "sp", None),
        P(),
        P(),
        P(),
        P(),
        P(),
        P(("grp", "sp"), "tp", None),
        P(("grp", "sp"), "tp", None),
    )
    return jax.shard_map(
        functools.partial(local, mesh.shape["sp"], mesh.shape["tp"]),
        mesh=mesh,
        in_specs=placed,
        out_specs=(
            P(("grp", "sp"), "tp", None, None),
            P(("grp", "sp"), "tp", None, None),
            P(("grp", "sp"), None, None),
            P(("grp", "sp"), "tp", None),
        ),
        check_vma=False,
    )
```

```python
import functools

import jax
import jax.numpy as jnp
import numpy as np
from jax import lax
from jax.experimental import pallas as pl
from jax.experimental.pallas import tpu as pltpu
from jax.sharding import PartitionSpec as P

norm_epsilon = 1e-06
rope_base = 10000.0
f32, bf16 = jnp.float32, jnp.bfloat16
ANY = pl.BlockSpec(memory_space=pl.ANY)
VMEM = pl.BlockSpec(memory_space=pltpu.VMEM)


def turns(positions, half):
    exponent = np.arange(0, 2 * half, 2, dtype=np.float32) / np.float32(2 * half)
    frequency = np.float32(1.0) / np.power(np.float32(rope_base), exponent)
    angles = frequency[:, None] * np.asarray(positions, np.float32)[None, :]
    return np.concatenate([np.cos(angles), np.sin(angles)]).astype(np.float32)


def project_kernel(chunks, x, w, r, gain, turn, out, xs, ws, rs, gs, ts, sems):
    seqs, pos, width = x.shape
    half = r.shape[0] // 2
    step = width // chunks
    copies = []
    for c in range(chunks):
        part = pl.ds(c * step, step)
        copies.append(pltpu.make_async_copy(w.at[part], ws.at[part], sems.at[c]))
        copies.append(pltpu.make_async_copy(x.at[:, :, part], xs.at[:, :, part], sems.at[chunks + c]))
    place = pl.ds(pl.multiple_of(lax.axis_index("sp") * pos, pos), pos)
    copies.append(pltpu.make_async_copy(r, rs, sems.at[2 * chunks]))
    copies.append(pltpu.make_async_copy(gain, gs, sems.at[2 * chunks + 1]))
    copies.append(pltpu.make_async_copy(turn.at[:, place], ts, sems.at[2 * chunks + 2]))
    for copy in copies:
        copy.start()
    latents = [None] * seqs
    for c in range(chunks):
        copies[2 * c].wait()
        copies[2 * c + 1].wait()
        for s in range(seqs):
            term = jnp.dot(
                xs[s, :, c * step : (c + 1) * step],
                ws[c * step : (c + 1) * step, :],
                preferred_element_type=f32,
            )
            latents[s] = term if c == 0 else latents[s] + term
    for copy in copies[2 * chunks :]:
        copy.wait()
    cosine, sine = ts[:half], ts[half:]
    for s in range(seqs):
        latent = latents[s]
        square = jnp.mean(latent * latent, axis=-1, keepdims=True)
        normed = latent * lax.rsqrt(square + norm_epsilon) * gs[...]
        out[s, :pos, :] = normed.astype(bf16)
        raw = lax.dot_general(
            rs[...], xs[s], (((1,), (1,)), ((), ())), preferred_element_type=f32
        )
        front, back = raw[:half], raw[half:]
        out[s, pos:, :pos] = (front * cosine - back * sine).astype(bf16)
        out[s, pos:, pos : 2 * pos] = (front * sine + back * cosine).astype(bf16)


def project(tokens, kv_down, rope_t, gain, sp_count):
    seqs, pos, width = tokens.shape
    latent = kv_down.shape[1]
    half = rope_t.shape[0] // 2
    assert 2 * pos == latent
    chunks = 4
    turn = jnp.asarray(turns(np.arange(pos * sp_count), half))
    return pl.pallas_call(
        functools.partial(project_kernel, chunks),
        out_shape=pltpu.VMEM((seqs, pos + half, latent), bf16),
        in_specs=[ANY] * 5,
        out_specs=VMEM,
        scratch_shapes=[
            pltpu.VMEM(tokens.shape, bf16),
            pltpu.VMEM(kv_down.shape, bf16),
            pltpu.VMEM(rope_t.shape, bf16),
            pltpu.VMEM((1, latent), f32),
            pltpu.VMEM((2 * half, pos), f32),
            pltpu.SemaphoreType.DMA((2 * chunks + 3,)),
        ],
        name="project",
        cost_estimate=pl.CostEstimate(
            flops=2 * seqs * pos * width * (latent + 2 * half),
            bytes_accessed=2 * (tokens.size + kv_down.size + seqs * pos * latent),
            transcendentals=0,
        ),
    )(tokens, kv_down, rope_t, gain[None], turn)


def absorb_kernel(k, last, two, heads, scale, place, relayed, *refs):
    first = k == 0
    block, refs = refs[0], refs[1:]
    if two:
        other, refs = refs[0], refs[1:]
    w, q, qr, refs = refs[0], refs[1], refs[2], refs[3:]
    if not first:
        state, refs = refs[0], refs[4:]
    keys, values, ropes, end, kv, rope, read_out, sems = refs
    half = qr.shape[1] // 2
    pos = block.shape[0] - half
    wide = w.shape[1] // 2
    head = wide // heads
    place = pl.ds(pl.multiple_of(place() * pos, pos), pos)
    held = block[...]
    if two:
        held = jnp.where(relayed() == 1, other[...], held)
    rope[:half] = held[pos:, :pos]
    rope[half:] = held[pos:, pos : 2 * pos]
    copies = [pltpu.make_async_copy(rope, ropes.at[:, place], sems.at[2 * heads])]
    copies[0].start()
    x = held[:pos]
    made = []
    for i, cache in enumerate((keys, values)):
        both = jnp.dot(x, w[:, i * wide : (i + 1) * wide], preferred_element_type=f32)
        both = both.astype(bf16)
        made.append(both)
        for h in range(heads):
            n = i * heads + h
            kv[n] = both[:, h * head : (h + 1) * head]
            copies.append(pltpu.make_async_copy(kv.at[n], cache.at[h, place], sems.at[n]))
            copies[-1].start()
    key, value = made
    scores = lax.dot_general(q[...], key, (((1,), (1,)), ((), ())), preferred_element_type=f32)
    scores = scores + jnp.dot(qr[...], rope[...], preferred_element_type=f32)
    scores = scores * scale
    peak = jnp.max(scores, axis=-1, keepdims=True)
    if not first:
        old_peak = state[0, :, :1]
        peak = jnp.maximum(peak, old_peak)
    terms = jnp.exp(scores - peak)
    total = jnp.sum(terms, axis=-1, keepdims=True)
    high = terms.astype(bf16)
    low = (terms - high.astype(f32)).astype(bf16)
    read = jnp.dot(high, value, preferred_element_type=f32) + jnp.dot(
        low, value, preferred_element_type=f32
    )
    row = lax.broadcasted_iota(jnp.int32, (heads, 1), 0)
    mine = jnp.zeros((heads, head), f32)
    for h in range(heads):
        mine = mine + jnp.where(row == h, read[:, h * head : (h + 1) * head], 0.0)
    if not first:
        fade = jnp.exp(old_peak - peak)
        total = total + fade * state[1, :, :1]
        mine = mine + fade * state[2]
    if last:
        read_out[...] = (mine / total).astype(bf16)
        copies.append(pltpu.make_async_copy(read_out, end, sems.at[2 * heads + 1]))
        copies[-1].start()
    else:
        end[0] = jnp.broadcast_to(peak, mine.shape)
        end[1] = jnp.broadcast_to(total, mine.shape)
        end[2] = mine
    for copy in copies:
        copy.wait()


def absorb(k, blocks, heads, scale, lookups, either, w, q, qr, held):
    first, last = k == 0, k == blocks - 1
    latent = w.shape[0]
    half = qr.shape[1] // 2
    pos = either[0].shape[0] - half
    head = w.shape[1] // (2 * heads)
    caches = [
        jax.ShapeDtypeStruct((heads, blocks * pos, head), bf16),
        jax.ShapeDtypeStruct((heads, blocks * pos, head), bf16),
        jax.ShapeDtypeStruct((2 * half, blocks * pos), bf16),
    ]
    end = jax.ShapeDtypeStruct((heads, head), bf16) if last else jax.ShapeDtypeStruct(
        (3, heads, head), f32
    )
    extra = [] if first else [held[3], *held[:3]]
    base = 4 + len(either)
    return pl.pallas_call(
        functools.partial(absorb_kernel, k, last, len(either) == 2, heads, scale, *lookups),
        out_shape=[*caches, end],
        in_specs=[VMEM] * (len(either) + 3)
        + ([] if first else [VMEM, ANY, ANY, ANY]),
        out_specs=[ANY, ANY, ANY, ANY if last else VMEM],
        input_output_aliases={} if first else {base: 0, base + 1: 1, base + 2: 2},
        scratch_shapes=[
            pltpu.VMEM((2 * heads, pos, head), bf16),
            pltpu.VMEM((2 * half, pos), bf16),
            pltpu.VMEM((heads, head), bf16),
            pltpu.SemaphoreType.DMA((2 * heads + 2,)),
        ],
        compiler_params=pltpu.CompilerParams(vmem_limit_bytes=8 * 2**20),
        name="absorb",
        cost_estimate=pl.CostEstimate(
            flops=4 * pos * latent * heads * head,
            bytes_accessed=2 * (either[0].size + w.size) + 4 * pos * heads * head,
            transcendentals=heads * pos,
        ),
    )(*either, w, q, qr, *extra)


def rotated_query(query_rope, position):
    half = query_rope.shape[-1] // 2
    turn = turns([position], half)[:, 0]
    cosine, sine = jnp.asarray(turn[:half]), jnp.asarray(turn[half:])
    front, back = query_rope[..., :half].astype(f32), query_rope[..., half:].astype(f32)
    turned = [front * cosine - back * sine, front * sine + back * cosine]
    return jnp.concatenate(turned, axis=-1).astype(bf16)


def lookup(table, tp_count):
    spot = lax.axis_index("sp") * tp_count + lax.axis_index("tp")
    bits = max(max(table).bit_length(), 1)
    each = 31 // bits
    value = jnp.int32(0)
    for i in range(0, len(table), each):
        word = sum(v << (j * bits) for j, v in enumerate(table[i : i + each]))
        if word:
            shift = jnp.clip(spot - i, 0, each - 1) * bits
            piece = lax.shift_right_logical(jnp.int32(word), shift) & (2**bits - 1)
            value = value + jnp.where((spot >= i) & (spot < i + each), piece, 0)
    return value


ORDER = (
    ((3, 0, 1, 2), (1, 2, 0, 3), (0, 3, 2, 1), (2, 1, 3, 0)),
    ((1, 3, 2, 0), (2, 0, 3, 1), (0, 2, 1, 3), (3, 1, 0, 2)),
    ((1, 0, 2, 3), (2, 3, 0, 1), (3, 2, 1, 0), (0, 1, 3, 2)),
    ((1, 0, 2, 3), (3, 2, 1, 0), (0, 1, 3, 2), (2, 3, 0, 1)),
)
RELAYS = (
    ((0, 2, 3), (1, 3, 2), (2, 0, 1), (3, 1, 0)),
)


def plan(sp_count, tp_count, seqs):
    place = np.zeros((sp_count, tp_count, sp_count), np.int32)
    relayed = np.zeros_like(place)
    lane = np.zeros_like(place)
    rounds = [[] for _ in range(sp_count)]
    relays = []
    special = seqs == 1 and sp_count == 4
    if special:
        for step in RELAYS:
            relays.append([(s * tp_count + t, s * tp_count + to) for s, t, to in step])
            for s, t, to in step:
                relayed[s, to, sp_count - len(RELAYS) + len(relays) - 1] = 1
    fold = sp_count // 2
    for s in range(sp_count):
        for t in range(tp_count):
            for k in range(sp_count):
                if special:
                    source = ORDER[s][t][k]
                else:
                    rank = (s % seqs * tp_count + t - k) % sp_count
                    source = rank % fold * 2 + rank // fold
                place[s, t, k] = source
                lane[source, s // seqs, k] = s % seqs
                if not relayed[s, t, k]:
                    rounds[k].append((source * tp_count + s // seqs, s * tp_count + t))
    return rounds, relays, place, relayed, lane


def local(sp_count, tp_count, tokens, kv_down, rope_down, kv_gain, key_up, value_up, query_nope, query_rope):
    seqs, pos, _ = tokens.shape
    assert seqs * tp_count == sp_count and sp_count % 2 == 0
    latent, head_count, key_width = key_up.shape
    heads = head_count // tp_count
    rounds, relays, place, relayed, lane = plan(sp_count, tp_count, seqs)
    blocks = project(tokens, kv_down, rope_down.T, kv_gain, sp_count)

    def own(table):
        return functools.partial(lookup, table.reshape(-1).tolist(), tp_count)

    start = lax.axis_index("tp") * heads
    w = jnp.concatenate(
        [
            lax.dynamic_slice_in_dim(up, start, heads, 1).reshape(latent, -1)
            for up in (key_up, value_up)
        ],
        axis=1,
    )
    arrived = []
    for k, pairs in enumerate(rounds):
        block = blocks[0]
        if seqs > 1:
            block = lax.dynamic_index_in_dim(blocks, own(lane[:, :, k])(), 0, keepdims=False)
        arrived.append(lax.ppermute(block, ("sp", "tp"), pairs))

    eye = jnp.eye(heads, dtype=bf16)
    q = (query_nope[0][:, None, :] * eye[:, :, None]).reshape(heads, heads * key_width)
    qr = rotated_query(query_rope[0], pos * sp_count)
    scale = (key_width + query_rope.shape[-1]) ** (-0.5)
    passed = [lax.ppermute(arrived[j], ("sp", "tp"), pairs) for j, pairs in enumerate(relays)]
    held = None
    for k in range(sp_count):
        either = [arrived[k]]
        if k >= sp_count - len(relays):
            either.append(passed[k - sp_count + len(relays)])
        lookups = own(place[:, :, k]), own(relayed[:, :, k])
        held = absorb(k, sp_count, heads, scale, lookups, either, w, q, qr, held)
    keys, values, ropes, read = held
    return keys[None], values[None], ropes.T[None], read[None]


def solution(mesh):
    placed = (
        P(("grp", "tp"), "sp", None),
        P(),
        P(),
        P(),
        P(),
        P(),
        P(("grp", "sp"), "tp", None),
        P(("grp", "sp"), "tp", None),
    )
    return jax.shard_map(
        functools.partial(local, mesh.shape["sp"], mesh.shape["tp"]),
        mesh=mesh,
        in_specs=placed,
        out_specs=(
            P(("grp", "sp"), "tp", None, None),
            P(("grp", "sp"), "tp", None, None),
            P(("grp", "sp"), None, None),
            P(("grp", "sp"), "tp", None),
        ),
        check_vma=False,
    )
```

```python
import functools

import jax
import jax.numpy as jnp
import numpy as np
from jax import lax
from jax.experimental import pallas as pl
from jax.experimental.pallas import tpu as pltpu
from jax.sharding import PartitionSpec as P

norm_epsilon = 1e-06
rope_base = 10000.0
f32, bf16 = jnp.float32, jnp.bfloat16
ANY = pl.BlockSpec(memory_space=pl.ANY)
VMEM = pl.BlockSpec(memory_space=pltpu.VMEM)


def turns(positions, half):
    exponent = np.arange(0, 2 * half, 2, dtype=np.float32) / np.float32(2 * half)
    frequency = np.float32(1.0) / np.power(np.float32(rope_base), exponent)
    angles = frequency[:, None] * np.asarray(positions, np.float32)[None, :]
    return np.concatenate([np.cos(angles), np.sin(angles)]).astype(np.float32)


def project_kernel(chunks, x, w, r, gain, turn, out, xs, ws, rs, gs, ts, sems):
    seqs, pos, width = x.shape
    half = r.shape[0] // 2
    step = width // chunks
    copies = []
    for c in range(chunks):
        part = pl.ds(c * step, step)
        copies.append(pltpu.make_async_copy(w.at[part], ws.at[part], sems.at[c]))
        copies.append(pltpu.make_async_copy(x.at[:, :, part], xs.at[:, :, part], sems.at[chunks + c]))
    place = pl.ds(pl.multiple_of(lax.axis_index("sp") * pos, pos), pos)
    copies.append(pltpu.make_async_copy(r, rs, sems.at[2 * chunks]))
    copies.append(pltpu.make_async_copy(gain, gs, sems.at[2 * chunks + 1]))
    copies.append(pltpu.make_async_copy(turn.at[:, place], ts, sems.at[2 * chunks + 2]))
    for copy in copies:
        copy.start()
    latents = [None] * seqs
    for c in range(chunks):
        copies[2 * c].wait()
        copies[2 * c + 1].wait()
        for s in range(seqs):
            term = jnp.dot(
                xs[s, :, c * step : (c + 1) * step],
                ws[c * step : (c + 1) * step, :],
                preferred_element_type=f32,
            )
            latents[s] = term if c == 0 else latents[s] + term
    for copy in copies[2 * chunks :]:
        copy.wait()
    cosine, sine = ts[:half], ts[half:]
    for s in range(seqs):
        latent = latents[s]
        square = jnp.mean(latent * latent, axis=-1, keepdims=True)
        normed = latent * lax.rsqrt(square + norm_epsilon) * gs[...]
        out[s, :pos, :] = normed.astype(bf16)
        raw = lax.dot_general(
            rs[...], xs[s], (((1,), (1,)), ((), ())), preferred_element_type=f32
        )
        front, back = raw[:half], raw[half:]
        out[s, pos:, :pos] = (front * cosine - back * sine).astype(bf16)
        out[s, pos:, pos : 2 * pos] = (front * sine + back * cosine).astype(bf16)


def project(tokens, kv_down, rope_t, gain, sp_count):
    seqs, pos, width = tokens.shape
    latent = kv_down.shape[1]
    half = rope_t.shape[0] // 2
    assert 2 * pos == latent
    chunks = 4
    turn = jnp.asarray(turns(np.arange(pos * sp_count), half))
    return pl.pallas_call(
        functools.partial(project_kernel, chunks),
        out_shape=pltpu.VMEM((seqs, pos + half, latent), bf16),
        in_specs=[ANY] * 5,
        out_specs=VMEM,
        scratch_shapes=[
            pltpu.VMEM(tokens.shape, bf16),
            pltpu.VMEM(kv_down.shape, bf16),
            pltpu.VMEM(rope_t.shape, bf16),
            pltpu.VMEM((1, latent), f32),
            pltpu.VMEM((2 * half, pos), f32),
            pltpu.SemaphoreType.DMA((2 * chunks + 3,)),
        ],
        name="project",
        cost_estimate=pl.CostEstimate(
            flops=2 * seqs * pos * width * (latent + 2 * half),
            bytes_accessed=2 * (tokens.size + kv_down.size + seqs * pos * latent),
            transcendentals=0,
        ),
    )(tokens, kv_down, rope_t, gain[None], turn)


def absorb_kernel(k, last, two, heads, scale, place, relayed, *refs):
    first = k == 0
    block, refs = refs[0], refs[1:]
    if two:
        other, refs = refs[0], refs[1:]
    w, q, qr, refs = refs[0], refs[1], refs[2], refs[3:]
    if not first:
        state, refs = refs[0], refs[4:]
    keys, values, ropes, end, kv, rope, read_out, sems = refs
    half = qr.shape[1] // 2
    pos = block.shape[0] - half
    wide = w.shape[1] // 2
    head = wide // heads
    place = pl.ds(pl.multiple_of(place() * pos, pos), pos)
    held = block[...]
    if two:
        held = jnp.where(relayed() == 1, other[...], held)
    rope[:half] = held[pos:, :pos]
    rope[half:] = held[pos:, pos : 2 * pos]
    copies = [pltpu.make_async_copy(rope, ropes.at[:, place], sems.at[2 * heads])]
    copies[0].start()
    x = held[:pos]

    def fill(i, cache):
        both = jnp.dot(x, w[:, i * wide : (i + 1) * wide], preferred_element_type=f32)
        both = both.astype(bf16)
        for h in range(heads):
            n = i * heads + h
            kv[n] = both[:, h * head : (h + 1) * head]
            copies.append(pltpu.make_async_copy(kv.at[n], cache.at[h, place], sems.at[n]))
            copies[-1].start()
        return both

    key = fill(0, keys)
    value = None if last else fill(1, values)
    scores = lax.dot_general(q[...], key, (((1,), (1,)), ((), ())), preferred_element_type=f32)
    scores = scores + jnp.dot(qr[...], rope[...], preferred_element_type=f32)
    scores = scores * scale
    peak = jnp.max(scores, axis=-1, keepdims=True)
    if not first:
        old_peak = state[0, :, :1]
        peak = jnp.maximum(peak, old_peak)
    terms = jnp.exp(scores - peak)
    total = jnp.sum(terms, axis=-1, keepdims=True)
    row = lax.broadcasted_iota(jnp.int32, (2 * heads, 1), 0)
    high = terms.astype(bf16).astype(f32)
    split = jnp.where(row < heads, high, terms - high).astype(bf16)
    value = fill(1, values) if last else value
    read = jnp.dot(split, value, preferred_element_type=f32)
    mine = jnp.zeros((2 * heads, head), f32)
    for h in range(heads):
        of_head = (row == h) | (row == heads + h)
        mine = mine + jnp.where(of_head, read[:, h * head : (h + 1) * head], 0.0)
    if not first:
        fade = jnp.exp(old_peak - peak)
        total = total + fade * state[1, :, :1]
        mine = mine + fade * state[2]
    if last:
        read_out[...] = ((mine[:heads] + mine[heads:]) / total[:heads]).astype(bf16)
        copies.append(pltpu.make_async_copy(read_out, end, sems.at[2 * heads + 1]))
        copies[-1].start()
    else:
        end[0] = jnp.broadcast_to(peak, mine.shape)
        end[1] = jnp.broadcast_to(total, mine.shape)
        end[2] = mine
    for copy in copies:
        copy.wait()


def absorb(k, blocks, heads, scale, lookups, either, w, q, qr, held):
    first, last = k == 0, k == blocks - 1
    latent = w.shape[0]
    half = qr.shape[1] // 2
    pos = either[0].shape[0] - half
    head = w.shape[1] // (2 * heads)
    caches = [
        jax.ShapeDtypeStruct((heads, blocks * pos, head), bf16),
        jax.ShapeDtypeStruct((heads, blocks * pos, head), bf16),
        jax.ShapeDtypeStruct((2 * half, blocks * pos), bf16),
    ]
    end = jax.ShapeDtypeStruct((heads, head), bf16) if last else jax.ShapeDtypeStruct(
        (3, 2 * heads, head), f32
    )
    extra = [] if first else [held[3], *held[:3]]
    base = 4 + len(either)
    return pl.pallas_call(
        functools.partial(absorb_kernel, k, last, len(either) == 2, heads, scale, *lookups),
        out_shape=[*caches, end],
        in_specs=[VMEM] * (len(either) + 3)
        + ([] if first else [VMEM, ANY, ANY, ANY]),
        out_specs=[ANY, ANY, ANY, ANY if last else VMEM],
        input_output_aliases={} if first else {base: 0, base + 1: 1, base + 2: 2},
        scratch_shapes=[
            pltpu.VMEM((2 * heads, pos, head), bf16),
            pltpu.VMEM((2 * half, pos), bf16),
            pltpu.VMEM((heads, head), bf16),
            pltpu.SemaphoreType.DMA((2 * heads + 2,)),
        ],
        compiler_params=pltpu.CompilerParams(vmem_limit_bytes=8 * 2**20),
        name="absorb",
        cost_estimate=pl.CostEstimate(
            flops=4 * pos * latent * heads * head,
            bytes_accessed=2 * (either[0].size + w.size) + 4 * pos * heads * head,
            transcendentals=heads * pos,
        ),
    )(*either, w, q, qr, *extra)


def rotated_query(query_rope, position):
    half = query_rope.shape[-1] // 2
    turn = turns([position], half)[:, 0]
    cosine, sine = jnp.asarray(turn[:half]), jnp.asarray(turn[half:])
    front, back = query_rope[..., :half].astype(f32), query_rope[..., half:].astype(f32)
    turned = [front * cosine - back * sine, front * sine + back * cosine]
    return jnp.concatenate(turned, axis=-1).astype(bf16)


def lookup(table, tp_count):
    spot = lax.axis_index("sp") * tp_count + lax.axis_index("tp")
    bits = max(max(table).bit_length(), 1)
    each = 31 // bits
    value = jnp.int32(0)
    for i in range(0, len(table), each):
        word = sum(v << (j * bits) for j, v in enumerate(table[i : i + each]))
        if word:
            shift = jnp.clip(spot - i, 0, each - 1) * bits
            piece = lax.shift_right_logical(jnp.int32(word), shift) & (2**bits - 1)
            value = value + jnp.where((spot >= i) & (spot < i + each), piece, 0)
    return value


ORDER = (
    ((3, 0, 1, 2), (1, 2, 0, 3), (0, 3, 2, 1), (2, 1, 3, 0)),
    ((1, 3, 2, 0), (2, 0, 3, 1), (0, 2, 1, 3), (3, 1, 0, 2)),
    ((1, 0, 2, 3), (2, 3, 0, 1), (3, 2, 1, 0), (0, 1, 3, 2)),
    ((1, 0, 2, 3), (3, 2, 1, 0), (0, 1, 3, 2), (2, 3, 0, 1)),
)
RELAYS = (
    ((0, 2, 3), (1, 3, 2), (2, 0, 1), (3, 1, 0)),
)


def plan(sp_count, tp_count, seqs):
    place = np.zeros((sp_count, tp_count, sp_count), np.int32)
    relayed = np.zeros_like(place)
    lane = np.zeros_like(place)
    rounds = [[] for _ in range(sp_count)]
    relays = []
    special = seqs == 1 and sp_count == 4
    if special:
        for step in RELAYS:
            relays.append([(s * tp_count + t, s * tp_count + to) for s, t, to in step])
            for s, t, to in step:
                relayed[s, to, sp_count - len(RELAYS) + len(relays) - 1] = 1
    fold = sp_count // 2
    for s in range(sp_count):
        for t in range(tp_count):
            for k in range(sp_count):
                if special:
                    source = ORDER[s][t][k]
                else:
                    rank = (s % seqs * tp_count + t - k) % sp_count
                    source = rank % fold * 2 + rank // fold
                place[s, t, k] = source
                lane[source, s // seqs, k] = s % seqs
                if not relayed[s, t, k]:
                    rounds[k].append((source * tp_count + s // seqs, s * tp_count + t))
    return rounds, relays, place, relayed, lane


def local(sp_count, tp_count, tokens, kv_down, rope_down, kv_gain, key_up, value_up, query_nope, query_rope):
    seqs, pos, _ = tokens.shape
    assert seqs * tp_count == sp_count and sp_count % 2 == 0
    latent, head_count, key_width = key_up.shape
    heads = head_count // tp_count
    rounds, relays, place, relayed, lane = plan(sp_count, tp_count, seqs)
    blocks = project(tokens, kv_down, rope_down.T, kv_gain, sp_count)

    def own(table):
        return functools.partial(lookup, table.reshape(-1).tolist(), tp_count)

    start = lax.axis_index("tp") * heads
    w = jnp.concatenate(
        [
            lax.dynamic_slice_in_dim(up, start, heads, 1).reshape(latent, -1)
            for up in (key_up, value_up)
        ],
        axis=1,
    )
    arrived = []
    for k, pairs in enumerate(rounds):
        block = blocks[0]
        if seqs > 1:
            block = lax.dynamic_index_in_dim(blocks, own(lane[:, :, k])(), 0, keepdims=False)
        arrived.append(lax.ppermute(block, ("sp", "tp"), pairs))

    eye = jnp.eye(heads, dtype=bf16)
    q = (query_nope[0][:, None, :] * eye[:, :, None]).reshape(heads, heads * key_width)
    q = jnp.concatenate([q, q])
    qr = rotated_query(query_rope[0], pos * sp_count)
    qr = jnp.concatenate([qr, qr])
    scale = (key_width + query_rope.shape[-1]) ** (-0.5)
    passed = [lax.ppermute(arrived[j], ("sp", "tp"), pairs) for j, pairs in enumerate(relays)]
    held = None
    for k in range(sp_count):
        either = [arrived[k]]
        if k >= sp_count - len(relays):
            either.append(passed[k - sp_count + len(relays)])
        lookups = own(place[:, :, k]), own(relayed[:, :, k])
        held = absorb(k, sp_count, heads, scale, lookups, either, w, q, qr, held)
    keys, values, ropes, read = held
    return keys[None], values[None], ropes.T[None], read[None]


def solution(mesh):
    placed = (
        P(("grp", "tp"), "sp", None),
        P(),
        P(),
        P(),
        P(),
        P(),
        P(("grp", "sp"), "tp", None),
        P(("grp", "sp"), "tp", None),
    )
    return jax.shard_map(
        functools.partial(local, mesh.shape["sp"], mesh.shape["tp"]),
        mesh=mesh,
        in_specs=placed,
        out_specs=(
            P(("grp", "sp"), "tp", None, None),
            P(("grp", "sp"), "tp", None, None),
            P(("grp", "sp"), None, None),
            P(("grp", "sp"), "tp", None),
        ),
        check_vma=False,
    )
```

```python
import functools

import jax
import jax.numpy as jnp
import numpy as np
from jax import lax
from jax.experimental import pallas as pl
from jax.experimental.pallas import tpu as pltpu
from jax.sharding import PartitionSpec as P

norm_epsilon = 1e-06
rope_base = 10000.0
f32, bf16 = jnp.float32, jnp.bfloat16
ANY = pl.BlockSpec(memory_space=pl.ANY)
VMEM = pl.BlockSpec(memory_space=pltpu.VMEM)


def turns(positions, half):
    exponent = np.arange(0, 2 * half, 2, dtype=np.float32) / np.float32(2 * half)
    frequency = np.float32(1.0) / np.power(np.float32(rope_base), exponent)
    angles = frequency[:, None] * np.asarray(positions, np.float32)[None, :]
    return np.concatenate([np.cos(angles), np.sin(angles)]).astype(np.float32)


def project_kernel(chunks, x, w, r, gain, turn, out, xs, ws, rs, gs, ts, sems):
    seqs, pos, width = x.shape
    half = r.shape[0] // 2
    step = width // chunks
    copies = []
    for c in range(chunks):
        part = pl.ds(c * step, step)
        copies.append(pltpu.make_async_copy(w.at[part], ws.at[part], sems.at[c]))
        copies.append(pltpu.make_async_copy(x.at[:, :, part], xs.at[:, :, part], sems.at[chunks + c]))
    place = pl.ds(pl.multiple_of(lax.axis_index("sp") * pos, pos), pos)
    copies.append(pltpu.make_async_copy(r, rs, sems.at[2 * chunks]))
    copies.append(pltpu.make_async_copy(gain, gs, sems.at[2 * chunks + 1]))
    copies.append(pltpu.make_async_copy(turn.at[:, place], ts, sems.at[2 * chunks + 2]))
    for copy in copies:
        copy.start()
    latents = [None] * seqs
    for c in range(chunks):
        copies[2 * c].wait()
        copies[2 * c + 1].wait()
        for s in range(seqs):
            term = jnp.dot(
                xs[s, :, c * step : (c + 1) * step],
                ws[c * step : (c + 1) * step, :],
                preferred_element_type=f32,
            )
            latents[s] = term if c == 0 else latents[s] + term
    for copy in copies[2 * chunks :]:
        copy.wait()
    cosine, sine = ts[:half], ts[half:]
    for s in range(seqs):
        latent = latents[s]
        square = jnp.mean(latent * latent, axis=-1, keepdims=True)
        normed = latent * lax.rsqrt(square + norm_epsilon) * gs[...]
        out[s, :pos, :] = normed.astype(bf16)
        raw = lax.dot_general(
            rs[...], xs[s], (((1,), (1,)), ((), ())), preferred_element_type=f32
        )
        front, back = raw[:half], raw[half:]
        out[s, pos:, :pos] = (front * cosine - back * sine).astype(bf16)
        out[s, pos:, pos : 2 * pos] = (front * sine + back * cosine).astype(bf16)


def project(tokens, kv_down, rope_t, gain, sp_count):
    seqs, pos, width = tokens.shape
    latent = kv_down.shape[1]
    half = rope_t.shape[0] // 2
    assert 2 * pos == latent
    chunks = 4
    turn = jnp.asarray(turns(np.arange(pos * sp_count), half))
    return pl.pallas_call(
        functools.partial(project_kernel, chunks),
        out_shape=pltpu.VMEM((seqs, pos + half, latent), bf16),
        in_specs=[ANY] * 5,
        out_specs=VMEM,
        scratch_shapes=[
            pltpu.VMEM(tokens.shape, bf16),
            pltpu.VMEM(kv_down.shape, bf16),
            pltpu.VMEM(rope_t.shape, bf16),
            pltpu.VMEM((1, latent), f32),
            pltpu.VMEM((2 * half, pos), f32),
            pltpu.SemaphoreType.DMA((2 * chunks + 3,)),
        ],
        name="project",
        cost_estimate=pl.CostEstimate(
            flops=2 * seqs * pos * width * (latent + 2 * half),
            bytes_accessed=2 * (tokens.size + kv_down.size + seqs * pos * latent),
            transcendentals=0,
        ),
    )(tokens, kv_down, rope_t, gain[None], turn)


def absorb_kernel(k, last, two, heads, scale, place, relayed, *refs):
    first = k == 0
    block, refs = refs[0], refs[1:]
    if two:
        other, refs = refs[0], refs[1:]
    w, q, qr, refs = refs[:2], refs[2], refs[3], refs[4:]
    if not first:
        state, refs = refs[0], refs[4:]
    keys, values, ropes, end, kv, rope, read_out, sems = refs
    half = qr.shape[1] // 2
    pos = block.shape[0] - half
    wide = w[0].shape[1]
    head = wide // heads
    place = pl.ds(pl.multiple_of(place() * pos, pos), pos)
    held = block[...]
    if two:
        held = jnp.where(relayed() == 1, other[...], held)
    rope[:half] = held[pos:, :pos]
    rope[half:] = held[pos:, pos : 2 * pos]
    copies = [pltpu.make_async_copy(rope, ropes.at[:, place], sems.at[2 * heads])]
    copies[0].start()
    x = held[:pos]

    def fill(i, cache):
        both = jnp.dot(x, w[i][...], preferred_element_type=f32)
        both = both.astype(bf16)
        for h in range(heads):
            n = i * heads + h
            kv[n] = both[:, h * head : (h + 1) * head]
            copies.append(pltpu.make_async_copy(kv.at[n], cache.at[h, place], sems.at[n]))
            copies[-1].start()
        return both

    key = fill(0, keys)
    value = None if last else fill(1, values)
    scores = lax.dot_general(q[...], key, (((1,), (1,)), ((), ())), preferred_element_type=f32)
    scores = scores + jnp.dot(qr[...], rope[...], preferred_element_type=f32)
    scores = scores * scale
    peak = jnp.max(scores, axis=-1, keepdims=True)
    if not first:
        old_peak = state[0, :, :1]
        peak = jnp.maximum(peak, old_peak)
    terms = jnp.exp(scores - peak)
    total = jnp.sum(terms, axis=-1, keepdims=True)
    row = lax.broadcasted_iota(jnp.int32, (2 * heads, 1), 0)
    high = terms.astype(bf16).astype(f32)
    split = jnp.where(row < heads, high, terms - high).astype(bf16)
    value = fill(1, values) if last else value
    read = jnp.dot(split, value, preferred_element_type=f32)
    mine = jnp.zeros((2 * heads, head), f32)
    for h in range(heads):
        of_head = (row == h) | (row == heads + h)
        mine = mine + jnp.where(of_head, read[:, h * head : (h + 1) * head], 0.0)
    if not first:
        fade = jnp.exp(old_peak - peak)
        total = total + fade * state[1, :, :1]
        mine = mine + fade * state[2]
    if last:
        read_out[...] = ((mine[:heads] + mine[heads:]) / total[:heads]).astype(bf16)
        copies.append(pltpu.make_async_copy(read_out, end, sems.at[2 * heads + 1]))
        copies[-1].start()
    else:
        end[0] = jnp.broadcast_to(peak, mine.shape)
        end[1] = jnp.broadcast_to(total, mine.shape)
        end[2] = mine
    for copy in copies:
        copy.wait()


def absorb(k, blocks, heads, scale, lookups, either, w, q, qr, held):
    first, last = k == 0, k == blocks - 1
    latent = w[0].shape[0]
    half = qr.shape[1] // 2
    pos = either[0].shape[0] - half
    head = w[0].shape[1] // heads
    caches = [
        jax.ShapeDtypeStruct((heads, blocks * pos, head), bf16),
        jax.ShapeDtypeStruct((heads, blocks * pos, head), bf16),
        jax.ShapeDtypeStruct((2 * half, blocks * pos), bf16),
    ]
    end = jax.ShapeDtypeStruct((heads, head), bf16) if last else jax.ShapeDtypeStruct(
        (3, 2 * heads, head), f32
    )
    extra = [] if first else [held[3], *held[:3]]
    base = 5 + len(either)
    return pl.pallas_call(
        functools.partial(absorb_kernel, k, last, len(either) == 2, heads, scale, *lookups),
        out_shape=[*caches, end],
        in_specs=[VMEM] * (len(either) + 4)
        + ([] if first else [VMEM, ANY, ANY, ANY]),
        out_specs=[ANY, ANY, ANY, ANY if last else VMEM],
        input_output_aliases={} if first else {base: 0, base + 1: 1, base + 2: 2},
        scratch_shapes=[
            pltpu.VMEM((2 * heads, pos, head), bf16),
            pltpu.VMEM((2 * half, pos), bf16),
            pltpu.VMEM((heads, head), bf16),
            pltpu.SemaphoreType.DMA((2 * heads + 2,)),
        ],
        compiler_params=pltpu.CompilerParams(vmem_limit_bytes=8 * 2**20),
        name="absorb",
        cost_estimate=pl.CostEstimate(
            flops=4 * pos * latent * heads * head,
            bytes_accessed=2 * (either[0].size + 2 * w[0].size) + 4 * pos * heads * head,
            transcendentals=heads * pos,
        ),
    )(*either, *w, q, qr, *extra)


def rotated_query(query_rope, position):
    half = query_rope.shape[-1] // 2
    turn = turns([position], half)[:, 0]
    cosine, sine = jnp.asarray(turn[:half]), jnp.asarray(turn[half:])
    front, back = query_rope[..., :half].astype(f32), query_rope[..., half:].astype(f32)
    turned = [front * cosine - back * sine, front * sine + back * cosine]
    return jnp.concatenate(turned, axis=-1).astype(bf16)


def lookup(table, tp_count):
    spot = lax.axis_index("sp") * tp_count + lax.axis_index("tp")
    bits = max(max(table).bit_length(), 1)
    each = 31 // bits
    value = jnp.int32(0)
    for i in range(0, len(table), each):
        word = sum(v << (j * bits) for j, v in enumerate(table[i : i + each]))
        if word:
            shift = jnp.clip(spot - i, 0, each - 1) * bits
            piece = lax.shift_right_logical(jnp.int32(word), shift) & (2**bits - 1)
            value = value + jnp.where((spot >= i) & (spot < i + each), piece, 0)
    return value


ORDER = (
    ((3, 0, 1, 2), (1, 2, 0, 3), (0, 3, 2, 1), (2, 1, 3, 0)),
    ((1, 3, 2, 0), (2, 0, 3, 1), (0, 2, 1, 3), (3, 1, 0, 2)),
    ((1, 0, 2, 3), (2, 3, 0, 1), (3, 2, 1, 0), (0, 1, 3, 2)),
    ((1, 0, 2, 3), (3, 2, 1, 0), (0, 1, 3, 2), (2, 3, 0, 1)),
)
RELAYS = (
    ((0, 2, 3), (1, 3, 2), (2, 0, 1), (3, 1, 0)),
)


def plan(sp_count, tp_count, seqs):
    place = np.zeros((sp_count, tp_count, sp_count), np.int32)
    relayed = np.zeros_like(place)
    lane = np.zeros_like(place)
    rounds = [[] for _ in range(sp_count)]
    relays = []
    special = seqs == 1 and sp_count == 4
    if special:
        for step in RELAYS:
            relays.append([(s * tp_count + t, s * tp_count + to) for s, t, to in step])
            for s, t, to in step:
                relayed[s, to, sp_count - len(RELAYS) + len(relays) - 1] = 1
    fold = sp_count // 2
    for s in range(sp_count):
        for t in range(tp_count):
            for k in range(sp_count):
                if special:
                    source = ORDER[s][t][k]
                else:
                    rank = (s % seqs * tp_count + t - k) % sp_count
                    source = rank % fold * 2 + rank // fold
                place[s, t, k] = source
                lane[source, s // seqs, k] = s % seqs
                if not relayed[s, t, k]:
                    rounds[k].append((source * tp_count + s // seqs, s * tp_count + t))
    return rounds, relays, place, relayed, lane


def local(sp_count, tp_count, tokens, kv_down, rope_down, kv_gain, key_up, value_up, query_nope, query_rope):
    seqs, pos, _ = tokens.shape
    assert seqs * tp_count == sp_count and sp_count % 2 == 0
    latent, head_count, key_width = key_up.shape
    heads = head_count // tp_count
    rounds, relays, place, relayed, lane = plan(sp_count, tp_count, seqs)
    blocks = project(tokens, kv_down, rope_down.T, kv_gain, sp_count)

    def own(table):
        return functools.partial(lookup, table.reshape(-1).tolist(), tp_count)

    start = lax.axis_index("tp") * heads
    w = [
        lax.dynamic_slice_in_dim(up, start, heads, 1).reshape(latent, -1)
        for up in (key_up, value_up)
    ]
    arrived = []
    for k, pairs in enumerate(rounds):
        block = blocks[0]
        if seqs > 1:
            block = lax.dynamic_index_in_dim(blocks, own(lane[:, :, k])(), 0, keepdims=False)
        arrived.append(lax.ppermute(block, ("sp", "tp"), pairs))

    eye = jnp.eye(heads, dtype=bf16)
    q = (query_nope[0][:, None, :] * eye[:, :, None]).reshape(heads, heads * key_width)
    q = jnp.concatenate([q, q])
    qr = rotated_query(query_rope[0], pos * sp_count)
    qr = jnp.concatenate([qr, qr])
    scale = (key_width + query_rope.shape[-1]) ** (-0.5)
    passed = [lax.ppermute(arrived[j], ("sp", "tp"), pairs) for j, pairs in enumerate(relays)]
    held = None
    for k in range(sp_count):
        either = [arrived[k]]
        if k >= sp_count - len(relays):
            either.append(passed[k - sp_count + len(relays)])
        lookups = own(place[:, :, k]), own(relayed[:, :, k])
        held = absorb(k, sp_count, heads, scale, lookups, either, w, q, qr, held)
    keys, values, ropes, read = held
    return keys[None], values[None], ropes.T[None], read[None]


def solution(mesh):
    placed = (
        P(("grp", "tp"), "sp", None),
        P(),
        P(),
        P(),
        P(),
        P(),
        P(("grp", "sp"), "tp", None),
        P(("grp", "sp"), "tp", None),
    )
    return jax.shard_map(
        functools.partial(local, mesh.shape["sp"], mesh.shape["tp"]),
        mesh=mesh,
        in_specs=placed,
        out_specs=(
            P(("grp", "sp"), "tp", None, None),
            P(("grp", "sp"), "tp", None, None),
            P(("grp", "sp"), None, None),
            P(("grp", "sp"), "tp", None),
        ),
        check_vma=False,
    )
```
